32 devices in a mesh: grp: 2 (over y), kv: 4 (over z), tp: 4 (over x, core).
Axes of the slice: x: 2, y: 2, z: 4, core: 2. Of those that a mesh axis runs over, the one named last changes fastest.
Arguments:
- hidden: bfloat16 [256, 4096], P('grp', 'kv'), parts along dimension 0, may hold values from -64 to 64
- norm_gain: bfloat16 [4096], replicated, may hold values from 0.099609375 to 1.8984375
- w_query: bfloat16 [4096, 2048], P('kv', 'tp'), may hold values from -0.09375 to 0.09375
- w_key: bfloat16 [4096, 2048], P('kv', 'tp'), may hold values from -0.09375 to 0.09375
- w_value: bfloat16 [4096, 2048], P('kv', 'tp'), may hold values from -0.09375 to 0.09375
- w_gate: bfloat16 [4096, 2048], P('kv', 'tp'), may hold values from -0.09375 to 0.09375
- w_decay: bfloat16 [4096, 16], P(None, 'tp'), may hold values from -0.09375 to 0.09375
- w_write: bfloat16 [4096, 16], P(None, 'tp'), may hold values from -0.09375 to 0.09375
- decay_rate: float32 [16], P('tp'), may hold values from 0.02 to 1
- head_gain: bfloat16 [128], replicated, may hold values from 0.099609375 to 1.8984375
- w_output: bfloat16 [2048, 4096], P('tp', 'kv'), may hold values from -0.125 to 0.125
- state: float32 [64, 16, 16384], P(('grp', 'kv'), 'tp'), parts along dimension 0, may hold values from -6 to 6
- prev_keys: bfloat16 [64, 4, 2048], P(('grp', 'kv'), None, 'tp'), parts along dimension 0, may hold values from -6 to 6
- prev_values: bfloat16 [64, 4, 2048], P(('grp', 'kv'), None, 'tp'), parts along dimension 0, may hold values from -6 to 6
- prev_decay: float32 [64, 4, 16], P(('grp', 'kv'), None, 'tp'), parts along dimension 0, may hold values from -1 to -0.02
- prev_write: float32 [64, 4, 16], P(('grp', 'kv'), None, 'tp'), parts along dimension 0, may hold values from 0.05 to 0.95
- accepted: int32 [64], P(('grp', 'kv')), parts along dimension 0, may hold values from 0 to 4
Outputs:
- mixed: bfloat16 [256, 4096], P('grp', 'kv'), parts along dimension 0
- state_out: float32 [64, 16, 16384], P(('grp', 'kv'), 'tp'), parts along dimension 0
The draws below stay inside these ranges and needn't reach their ends.
There are 2 independent parts, one for each index of `grp`. The reference program is written for one: setup_inputs(seed, part) draws one part's arguments, and reference() takes and returns one part's arrays. A program takes and returns all parts, laid end to end along the dimension named above; an argument that names none is the same for every part. Nothing has to cross between parts.
All inputs are finite; a program needn't handle non-finite values.
Results may differ from the reference program's by a relative error of at most 0.0069.
Values may be sent and summed in bfloat16 or wider, within the bound.
A program may use at most 64 MiB of HBM per device.

```python
import math
import jax
import jax.numpy as jnp
from jax import lax

D = 4096
H = 16
DK = 128
PROP = 4
SEQS = 32
TOKENS = 128
HID = 2048


def draw_hidden(key, part):
    key_rows, key_cols, key_base = jax.random.split(jax.random.fold_in(key, 11), 3)
    columns = jnp.arange(D, dtype=jnp.float32)
    column_scale = jnp.exp(math.log(3.0) * columns / D + jax.random.uniform(key_cols, (D,), jnp.float32, -0.35, 0.35))
    row_scale = jnp.exp(jax.random.uniform(key_rows, (TOKENS, 1), jnp.float32, 0.0, math.log(10.0)))
    base = jax.random.normal(key_base, (TOKENS, D), jnp.float32)
    base = jnp.clip(base, -5.0, 5.0)
    return jnp.clip(0.3 * base * row_scale * column_scale, -64.0, 64.0).astype(jnp.bfloat16)


def plant(drawn, own_key, low, high):
    spot = [jax.random.randint(jax.random.fold_in(own_key, axis), (), 0, length) for axis, length in enumerate(drawn.shape)]
    widest = drawn.shape.index(max(drawn.shape))
    beside = spot[:widest] + [(spot[widest] + 1) % drawn.shape[widest]] + spot[widest + 1:]
    return drawn.at[tuple(spot)].set(low).at[tuple(beside)].set(high)


def block_levels(own_key, extent, pieces, least, top_value):
    loudness = 1.0
    for axis_at, parts in pieces:
        steps = jax.random.uniform(jax.random.fold_in(jax.random.fold_in(own_key, 6), axis_at), (parts,), jnp.float32, least / len(pieces), top_value / len(pieces))
        loudness = loudness * jnp.repeat(jnp.exp(steps), extent[axis_at] // parts).reshape((-1,) + (1,) * (len(extent) - 1 - axis_at))
    return loudness


def normal_values(key, shape, spread, most, cuts=(), kind=jnp.bfloat16):
    values = spread * jax.random.normal(key, shape, jnp.float32)
    if cuts:
        values = values * block_levels(key, shape, cuts, -0.22, 0.18)
    return jnp.clip(values, -most, most).astype(kind)


def setup_inputs(seed: int = 0, part: int = 0) -> dict:
    arg_keys = jax.random.split(jax.random.key(seed), 18)
    part_splits = jax.random.split(jax.random.fold_in(arg_keys[17], part), 18)
    return {
        "hidden": draw_hidden(jax.random.fold_in(jax.random.fold_in(arg_keys[17], part), 71), part),
        "norm_gain": jnp.clip(1.0 + 0.18 * jax.random.normal(arg_keys[1], (D,), jnp.float32), 0.099609375, 1.8984375).astype(jnp.bfloat16),
        "w_query": normal_values(arg_keys[2], (D, HID), D ** -0.5, 0.09375, ((0, 4), (1, 4))),
        "w_key": normal_values(arg_keys[3], (D, HID), D ** -0.5, 0.09375, ((0, 4), (1, 4))),
        "w_value": normal_values(arg_keys[4], (D, HID), D ** -0.5, 0.09375, ((0, 4), (1, 4))),
        "w_gate": normal_values(arg_keys[5], (D, HID), D ** -0.5, 0.09375, ((0, 4), (1, 4))),
        "w_decay": normal_values(arg_keys[6], (D, H), D ** -0.5, 0.09375, ((1, 4),)),
        "w_write": normal_values(arg_keys[7], (D, H), D ** -0.5, 0.09375, ((1, 4),)),
        "decay_rate": jnp.clip(jnp.exp(math.log(1.0) - 3.912023 * jax.random.uniform(arg_keys[8], (H,), jnp.float32) ** block_levels(arg_keys[8], (H,), ((0, 4),), -0.2, 0.2)), 0.02, 1.0),
        "head_gain": jnp.clip(1.0 + 0.18 * jax.random.normal(arg_keys[9], (DK,), jnp.float32), 0.099609375, 1.8984375).astype(jnp.bfloat16),
        "w_output": normal_values(arg_keys[10], (HID, D), HID ** -0.5, 0.125, ((0, 4), (1, 4))),
        "state": normal_values(part_splits[11], (SEQS, H, DK * DK), 1.0, 6.0, ((0, 4), (1, 4)), jnp.float32),
        "prev_keys": normal_values(part_splits[12], (SEQS, PROP, HID), 1.0, 6.0, ((0, 4), (2, 4))),
        "prev_values": normal_values(part_splits[13], (SEQS, PROP, HID), 1.0, 6.0, ((0, 4), (2, 4))),
        "prev_decay": jnp.clip(-1.0 + 0.98 * jax.random.uniform(part_splits[14], (SEQS, PROP, H), jnp.float32) ** block_levels(part_splits[14], (SEQS, PROP, H), ((0, 4), (2, 4)), -0.2, 0.2), -1.0, -0.02),
        "prev_write": jnp.clip(0.05 + 0.9 * jax.random.uniform(part_splits[15], (SEQS, PROP, H), jnp.float32) ** block_levels(part_splits[15], (SEQS, PROP, H), ((0, 4), (2, 4)), -0.2, 0.2), 0.05, 0.95),
        "accepted": plant(jax.random.randint(part_splits[16], (SEQS,), 0, PROP + 1), jax.random.fold_in(part_splits[16], 1), 0, PROP).astype(jnp.int32),
    }


EPSILON = 1e-06

def unit_rows(values):
    return values * lax.rsqrt(lax.optimization_barrier(jnp.sum(values * values, axis=-1, keepdims=True)) + EPSILON)

def update_state(state_matrix, single_key_row, value_row, decay_row, write_row):
    state_matrix = state_matrix * jnp.exp(decay_row)[:, None, None]
    draft_token = jnp.einsum('xaf,xa->xf', state_matrix, single_key_row, precision=lax.Precision.HIGHEST)
    return state_matrix + write_row[:, None, None] * single_key_row[:, :, None] * (value_row - draft_token)[:, None, :]

def one_sequence(items):
    carried_state, query_rows, keys, values, log_decay, writes, old_keys, old_values, old_decay, old_writes = items
    for token_position in range(PROP):
        carried_state = update_state(carried_state, old_keys[token_position], old_values[token_position], old_decay[token_position], old_writes[token_position])
    taken_state = carried_state
    produced_output = []
    for token_position in range(PROP):
        carried_state = update_state(carried_state, keys[token_position], values[token_position], log_decay[token_position], writes[token_position])
        produced_output.append(jnp.einsum('xaf,xa->xf', carried_state, query_rows[token_position], precision=lax.Precision.HIGHEST))
    return (taken_state, jnp.stack(produced_output))

def reference(hidden, norm_gain, w_query, w_key, w_value, w_gate, w_decay, w_write, decay_rate, head_gain, w_output, state, prev_keys, prev_values, prev_decay, prev_write, accepted):
    wide = hidden.astype(jnp.float32)
    inverse = lax.rsqrt(lax.optimization_barrier(jnp.mean(wide * wide, axis=1)) + EPSILON)
    scaled = (wide * norm_gain.astype(jnp.float32)).astype(jnp.bfloat16)
    seqs = state.shape[0]

    def project(weight):
        return jnp.dot(scaled, weight, preferred_element_type=jnp.float32) * inverse[:, None]

    def split_heads(block):
        return block.reshape(seqs, PROP, H, DK)
    query_rows = unit_rows(split_heads(project(w_query))) * DK ** (-0.5)
    keys = unit_rows(split_heads(project(w_key)))
    values = split_heads(project(w_value))
    gates = split_heads(project(w_gate))
    log_decay = (-decay_rate * jax.nn.softplus(project(w_decay))).reshape(seqs, PROP, H)
    writes = jax.nn.sigmoid(project(w_write)).reshape(seqs, PROP, H)
    taken = jnp.arange(PROP, dtype=jnp.int32)[None, :] < accepted[:, None]
    old_keys = unit_rows(split_heads(prev_keys.astype(jnp.float32)))
    old_values = split_heads(prev_values.astype(jnp.float32))
    old_decay = jnp.where(taken[:, :, None], prev_decay, 0.0)
    old_writes = jnp.where(taken[:, :, None], prev_write, 0.0)
    carried_state = state.reshape(seqs, H, DK, DK)
    taken_states, outputs = lax.map(one_sequence, (carried_state, query_rows, keys, values, log_decay, writes, old_keys, old_values, old_decay, old_writes))
    normed = outputs * lax.rsqrt(lax.optimization_barrier(jnp.mean(outputs * outputs, axis=-1, keepdims=True)) + EPSILON)
    normed = normed * head_gain.astype(jnp.float32) * jax.nn.silu(gates)
    heads_out = normed.reshape(seqs * PROP, H * DK).astype(jnp.bfloat16)
    total = jnp.dot(heads_out, w_output, preferred_element_type=jnp.float32)
    return (total.astype(jnp.bfloat16), taken_states.reshape(seqs, H, DK * DK))
```

```python
import functools

import jax
import jax.numpy as jnp
from jax import lax
from jax.experimental import pallas as pl
from jax.experimental.pallas import tpu as pltpu
from jax.sharding import PartitionSpec as P

EPSILON = 1e-06
F32 = jnp.float32
BF16 = jnp.bfloat16
MESH = pl.DeviceIdType.MESH
SMALL = 128
PACK = 32


def unit_rows(x):
    return x * lax.rsqrt(jnp.sum(x * x, axis=-1, keepdims=True) + EPSILON)


def dot(a, b):
    return jnp.dot(a, b, preferred_element_type=F32)


def dot_nt(a, b):
    return lax.dot_general(a, b, (((1,), (1,)), ((), ())), preferred_element_type=F32)


def kernel(
    n, tp, width_model,
    hidden_hbm, gain_hbm, wq_hbm, wk_hbm, wv_hbm, wg_hbm, wd_hbm, ww_hbm, rate_hbm, hgain_hbm,
    wo_hbm, state_hbm, pk_hbm, pv_hbm, pd_hbm, pw_hbm, acc_hbm,
    mixed_ref, sout_hbm,
    hid, wts, wo, send, recv, st, sb, newst, rows32, lbuf, ks, qs, dec, ho, gath,
    pf, pb, prx, pair, obuf,
    agg, recv2, spack, srecv,
    gain_ref, wd_ref, ww_ref, rate_ref, hgain_ref, pk_ref, pv_ref, pd_ref, pw_ref, acc_ref,
    ld_sem, sm_sem, st_sem, so_sem, rs_s, rs_r, r2_s, r2_r, sp_s, sp_r, ag_s, ag_r, p1_s, p1_r, p2_s, p2_r, p3_s, p3_r,
):
    me = lax.axis_index("kv")
    t = lax.axis_index("tp")
    core = lax.rem(t, 2)
    chip = t // 2
    chips = tp // 2
    partner = t + 1 - 2 * core
    tokens, local = hid.shape
    owned = tokens // n
    seqs = st.shape[0]
    heads = wd_ref.shape[0]
    width = wts.shape[2]
    dk = width // heads
    props = owned // seqs
    R = heads * owned
    pairs = n // 2
    packed = spack.shape[1]
    groups = owned // packed
    stride = SMALL // groups

    kv_peers = [lax.rem(me + d, n) for d in range(1, n)]
    tp_peers = [lax.rem(t + 2 * k, tp) for k in range(1, chips)]
    parity = lax.rem(me, 2)
    neighbour = me + 1 - 2 * parity
    offset = pl.multiple_of(me * local, local)

    def load(src, dst, sem):
        c = pltpu.make_async_copy(src, dst, sem)
        c.start()
        return c

    weights = (wk_hbm, wq_hbm, wv_hbm, wg_hbm)
    ld_h = load(hidden_hbm, hid, ld_sem.at[0])
    ld_gain = load(gain_hbm, gain_ref, sm_sem.at[0])
    barrier = pltpu.get_barrier_semaphore()
    for p in kv_peers:
        pl.semaphore_signal(barrier, inc=1, device_id={"kv": p}, device_id_type=MESH)
    for p in [partner] + tp_peers:
        pl.semaphore_signal(barrier, inc=1, device_id={"tp": p}, device_id_type=MESH)
    ld_w = [load(w, wts.at[i], ld_sem.at[1 + i]) for i, w in enumerate(weights)]
    ld_d = load(wd_hbm.at[:, pl.ds(offset, local)], wd_ref, sm_sem.at[1])
    ld_r = load(ww_hbm.at[:, pl.ds(offset, local)], ww_ref, sm_sem.at[2])
    ld_prev = [
        load(src, dst, sm_sem.at[3 + i])
        for i, (src, dst) in enumerate(
            [(pk_hbm, pk_ref), (pv_hbm, pv_ref), (pd_hbm, pd_ref), (pw_hbm, pw_ref), (acc_hbm, acc_ref)]
        )
    ]
    ld_s = [load(state_hbm.at[s], st.at[s], st_sem.at[s]) for s in range(seqs)]
    ld_late = [load(rate_hbm, rate_ref, sm_sem.at[8]), load(hgain_hbm, hgain_ref, sm_sem.at[9])]
    ld_o = load(wo_hbm, wo, ld_sem.at[5])

    ld_gain.wait()
    ld_h.wait()
    wide = hid[...].astype(F32)
    table = gain_ref[...].astype(F32)
    lanes = table.shape[1]
    count = local // lanes
    gain = []
    for j in range(count):
        row = table[j : j + 1]
        for k in range(1, n):
            row = jnp.where(me == k, table[k * count + j : k * count + j + 1], row)
        gain.append(row)
    scaled = (wide * jnp.concatenate(gain, axis=1)).astype(BF16)
    squares = jnp.sum(wide * wide, axis=1, keepdims=True)

    cols = [pl.ds(i * width, width) for i in range(4)]
    rs = []

    def block(index):
        return pl.ds(pl.multiple_of(index * owned, owned), owned)

    def to_neighbour(k, i):
        other = 2 * lax.rem(me // 2 + k, pairs) + 1 - parity
        c = pltpu.make_async_remote_copy(
            src_ref=send.at[block(other), cols[i]],
            dst_ref=recv.at[k, :, cols[i]],
            send_sem=rs_s.at[k, i],
            recv_sem=rs_r.at[k, i],
            device_id={"kv": neighbour},
            device_id_type=MESH,
        )
        c.start()
        return c

    def project(i):
        ld_w[i].wait()
        send[:, cols[i]] = dot(scaled, wts[i]).astype(BF16)
        if i == 0:
            pl.semaphore_wait(barrier, n - 1 + chips)
        rs.append([to_neighbour(k, i) for k in range(1, pairs)])

    project(0)
    ld_d.wait()
    ld_r.wait()
    wsmall = jnp.concatenate(
        [wd_ref[...].astype(F32), ww_ref[...].astype(F32), jnp.zeros((SMALL - 2 * heads, local), F32)],
        axis=0,
    ).astype(BF16)
    small = dot_nt(scaled, wsmall)
    lane = lax.broadcasted_iota(jnp.int32, (tokens, SMALL), 1)
    small = small + jnp.where(lane == 2 * heads, squares, 0.0)
    small = small.reshape(n, groups, packed, SMALL)
    tight = small[:, 0].reshape(n * packed, SMALL)
    for j in range(1, groups):
        tight = tight + pltpu.roll(small[:, j].reshape(n * packed, SMALL), j * stride, 1)
    spack[...] = tight.reshape(n, packed, SMALL)
    sp = []
    for d in range(1, n):
        c = pltpu.make_async_remote_copy(
            src_ref=spack.at[kv_peers[d - 1]],
            dst_ref=srecv.at[d - 1],
            send_sem=sp_s.at[d - 1],
            recv_sem=sp_r.at[d - 1],
            device_id={"kv": kv_peers[d - 1]},
            device_id_type=MESH,
        )
        c.start()
        sp.append(c)
    for i in range(1, 4):
        project(i)

    rs2 = []

    def relay(i):
        group = []
        for k in range(1, pairs):
            rs[i][k - 1].wait()
            target = lax.rem(me + 2 * k, n)
            pairsum = send[block(target), cols[i]].astype(F32) + recv[k, :, cols[i]].astype(F32)
            agg[k - 1, :, cols[i]] = pairsum.astype(BF16)
            c = pltpu.make_async_remote_copy(
                src_ref=agg.at[k - 1, :, cols[i]],
                dst_ref=recv2.at[k - 1, :, cols[i]],
                send_sem=r2_s.at[k - 1, i],
                recv_sem=r2_r.at[k - 1, i],
                device_id={"kv": target},
                device_id_type=MESH,
            )
            c.start()
            group.append(c)
        rs2.append(group)

    ri = lax.broadcasted_iota(jnp.int32, (R, R), 0)
    ci = lax.broadcasted_iota(jnp.int32, (R, R), 1)
    same = ri // props == ci // props
    lower = same & (ci <= ri)
    strict = same & (ci < ri)
    prow = ri % props
    per = heads * props
    src_row = ((ri // props) % heads) * owned + (ri // per) * props + ri % props
    perm = jnp.where(ci == src_row, 1.0, 0.0).astype(BF16)
    ek = lax.broadcasted_iota(jnp.int32, (dk, heads * dk), 0)
    ec = lax.broadcasted_iota(jnp.int32, (dk, heads * dk), 1)
    expand = jnp.where(ec // heads == ek, 1.0, 0.0).astype(BF16)
    lr = lax.broadcasted_iota(jnp.int32, (R, heads * dk), 0)
    lc = lax.broadcasted_iota(jnp.int32, (R, heads * dk), 1)
    lmask = (lr // props) % heads == lc % heads

    def spread_rows(xb):
        moved = dot(perm, xb).astype(BF16)
        return jnp.where(lmask, dot(moved, expand), 0.0).astype(BF16)

    def running(g):
        full = jnp.broadcast_to(g, (R, R))
        total = full
        for m in range(1, props):
            total = total + jnp.where(prow >= m, pltpu.roll(full, m, 0), 0.0)
        return full, total

    def decays(total):
        spread = total - total.T
        return jnp.where(lower, jnp.exp(jnp.where(lower, spread, 0.0)), 0.0)

    def coupling(kb, within, b):
        return jnp.where(strict, b * dot_nt(kb, kb) * within, 0.0).astype(BF16)

    def solve(a, rhs):
        u = rhs
        for _ in range(props - 1):
            u = rhs - dot(a, u.astype(BF16))
        return u

    def stack(get):
        return jnp.concatenate([get(h) for h in range(heads)], axis=0)

    def rows_of(ref):
        for s in range(seqs):
            rows32[pl.ds(s * props, props), :] = ref[s].astype(F32)
        return stack(lambda h: rows32[:, pl.ds(h * dk, dk)])

    for c in ld_prev:
        c.wait()
    kb = unit_rows(rows_of(pk_ref)).astype(BF16)
    values = rows_of(pv_ref)
    r16 = lax.broadcasted_iota(jnp.int32, (R, seqs), 0)
    c16 = lax.broadcasted_iota(jnp.int32, (R, seqs), 1)
    taken = ((r16 // props) % seqs == c16) & (r16 % props < acc_ref[...])
    pr = r16 % props
    hr = r16 // owned

    def column(ref):
        out = jnp.zeros((R, seqs), F32)
        for p in range(props):
            piece = ref[p]
            for h in range(heads):
                out = jnp.where((pr == p) & (hr == h), piece[h : h + 1, :], out)
        return jnp.sum(jnp.where(taken, out, 0.0), axis=1, keepdims=True)

    g = column(pd_ref)
    b = column(pw_ref)
    full, total = running(g)
    tail = jnp.zeros((R, R), F32)
    for m in range(1, props):
        tail = tail + jnp.where(prow < props - m, pltpu.roll(full, R - m, 0), 0.0)
    within = decays(total)
    dec[...] = jnp.broadcast_to(jnp.exp((total + tail)[:, :1]), (R, dk))
    lbuf[0] = spread_rows(kb)
    for s in range(seqs):
        ld_s[s].wait()
        prod = dot(lbuf[0, pl.ds(s * per, per), :], st[s].astype(BF16))
        for h in range(heads):
            ks[pl.ds(h * owned + s * props, props), :] = prod[h * props : (h + 1) * props]
    relay(0)
    relay(1)
    u = solve(coupling(kb, within, b), b * (values - jnp.exp(total[:, :1]) * ks[...]))
    u = dot(perm, (u * jnp.exp(tail[:, :1])).astype(BF16))
    urow = lax.broadcasted_iota(jnp.int32, (R, dk), 0)
    lt = lbuf[0].T
    relay(2)
    relay(3)
    direct = [to_neighbour(0, i) for i in range(4)]
    so = []
    for s in range(seqs):
        us = jnp.where(urow // per == s, u, 0.0).astype(BF16)
        pat = dec[pl.ds(s * props, heads, stride=owned), :]
        reps = 8 // heads if heads < 8 else 1
        pat = jnp.concatenate([pat] * reps, axis=0)
        old = st[s].reshape(heads * dk // pat.shape[0], pat.shape[0], dk)
        new = (old * pat[None]).reshape(heads * dk, dk) + dot(lt, us)
        newst[s] = new
        sb[s] = new.astype(BF16)
        so.append(load(newst.at[s], sout_hbm.at[s], so_sem.at[s]))

    own = block(me)

    def summed(i):
        x = send[own, cols[i]].astype(F32)
        x = x + recv[0, :, cols[i]].astype(F32)
        for k in range(1, pairs):
            x = x + recv2[k - 1, :, cols[i]].astype(F32)
        return x

    def arrive(i):
        for c in rs2[i]:
            c.wait()
        direct[i].wait()

    for c in sp + ld_late:
        c.wait()
    tight = spack[me]
    for d in range(1, n):
        tight = tight + srecv[d - 1]
    small = jnp.concatenate(
        [tight] + [pltpu.roll(tight, SMALL - j * stride, 1) for j in range(1, groups)], axis=0
    )
    inverse = lax.rsqrt(small[:, 2 * heads : 2 * heads + 1] / width_model + EPSILON)
    small = small * inverse
    inv = jnp.concatenate([inverse] * heads, axis=0)
    sm = jnp.concatenate([small] * heads, axis=0)
    sl = lax.broadcasted_iota(jnp.int32, (R, SMALL), 1)
    sh = lax.broadcasted_iota(jnp.int32, (R, SMALL), 0) // owned
    apre = jnp.sum(jnp.where(sl == sh, sm, 0.0), axis=1, keepdims=True)
    bpre = jnp.sum(jnp.where(sl == sh + heads, sm, 0.0), axis=1, keepdims=True)
    hl = lax.broadcasted_iota(jnp.int32, (R, heads), 1)
    hh = lax.broadcasted_iota(jnp.int32, (R, heads), 0) // owned
    rate = jnp.sum(jnp.where(hl == hh, rate_ref[...], 0.0), axis=1, keepdims=True)
    softplus = jnp.maximum(apre, 0.0) + jnp.log1p(jnp.exp(-jnp.abs(apre)))
    g = -rate * softplus
    b = jax.nn.sigmoid(bpre)
    full, total = running(g)
    within = decays(total)
    grow = jnp.exp(total[:, :1])

    def projected(i):
        x = summed(i)
        return stack(lambda h: x[:, h * dk : (h + 1) * dk]) * inv

    arrive(0)
    kb = unit_rows(projected(0)).astype(BF16)
    lbuf[0] = spread_rows(kb)
    couple = coupling(kb, within, b)
    arrive(1)
    qb = (unit_rows(projected(1)) * dk**-0.5).astype(BF16)
    lbuf[1] = spread_rows(qb)
    scores = (dot_nt(qb, kb) * within).astype(BF16)
    for s in range(seqs):
        lhs = jnp.concatenate(
            [lbuf[0, pl.ds(s * per, per), :], lbuf[1, pl.ds(s * per, per), :]], axis=0
        )
        prod = dot(lhs, sb[s])
        for h in range(heads):
            at = pl.ds(h * owned + s * props, props)
            ks[at, :] = prod[h * props : (h + 1) * props]
            qs[at, :] = prod[per + h * props : per + (h + 1) * props]
    arrive(2)
    u = solve(couple, b * (projected(2) - grow * ks[...]))
    read = grow * qs[...] + dot(scores, u.astype(BF16))
    normed = read * lax.rsqrt(jnp.mean(read * read, axis=-1, keepdims=True) + EPSILON)
    normed = normed * hgain_ref[...].astype(F32)
    arrive(3)
    gates = projected(3)
    normed = normed * (gates * jax.nn.sigmoid(gates))
    for h in range(heads):
        ho[:, pl.ds(h * dk, dk)] = normed[h * owned : (h + 1) * owned].astype(BF16)

    left, right = me, n - 1 - me
    most, least = jnp.maximum(left, right), jnp.minimum(left, right)
    way = jnp.where(right >= left, 1, -1)

    def ranked(k):
        past = jnp.maximum(k - (most - least), 0)
        far = jnp.where(k < most - least, most - k, least - past // 2)
        return me + far * way * (1 - 2 * lax.rem(past, 2))

    ag = []
    for k in range(n - 1):
        c = pltpu.make_async_remote_copy(
            src_ref=ho,
            dst_ref=gath.at[me],
            send_sem=ag_s.at[k],
            recv_sem=ag_r.at[me],
            device_id={"kv": ranked(k)},
            device_id_type=MESH,
        )
        c.start()
        ag.append(c)
    source = [me] + [ranked(k) for k in range(n - 2, -1, -1)]
    half = owned // 2
    first, second, third = [], [], []

    def multiply(d):
        if d:
            pltpu.make_async_remote_copy(
                src_ref=ho,
                dst_ref=gath.at[source[d]],
                send_sem=ag_s.at[0],
                recv_sem=ag_r.at[source[d]],
                device_id={"kv": source[d]},
                device_id_type=MESH,
            ).wait_recv()
        part = dot(gath[source[d]] if d else ho[...], wo[...])
        for e in range(2):
            piece = part[e * half : (e + 1) * half]
            pf[d, e] = piece
            pb[d, e] = piece.astype(BF16)
        c = pltpu.make_async_remote_copy(
            src_ref=pb.at[d, 1 - core],
            dst_ref=prx.at[d],
            send_sem=p1_s.at[d],
            recv_sem=p1_r.at[d],
            device_id={"tp": partner},
            device_id_type=MESH,
        )
        c.start()
        first.append(c)

    def cross(d):
        first[d].wait()
        pair[d, chip] = (pf[d, core] + prx[d].astype(F32)).astype(BF16)
        group = []
        for k in range(1, chips):
            c = pltpu.make_async_remote_copy(
                src_ref=pair.at[d, chip],
                dst_ref=pair.at[d, chip],
                send_sem=p2_s.at[d, k - 1],
                recv_sem=p2_r.at[d, k - 1],
                device_id={"tp": tp_peers[k - 1]},
                device_id_type=MESH,
            )
            c.start()
            group.append(c)
        second.append(group)

    def share(d):
        for c in second[d]:
            c.wait()
        x = pair[d, 0].astype(F32)
        for k in range(1, chips):
            x = x + pair[d, k].astype(F32)
        obuf[d, core] = x.astype(BF16)
        c = pltpu.make_async_remote_copy(
            src_ref=obuf.at[d, core],
            dst_ref=obuf.at[d, core],
            send_sem=p3_s.at[d],
            recv_sem=p3_r.at[d],
            device_id={"tp": partner},
            device_id_type=MESH,
        )
        c.start()
        third.append(c)

    def finish(d):
        third[d].wait()
        mixed_ref[source[d]] = obuf[d]

    ld_o.wait()
    multiply(0)
    cross(0)
    for d in range(1, n):
        multiply(d)
        if d >= 2:
            cross(d - 1)
        share(d - 1) if d == 1 else None
    cross(n - 1)
    for d in range(1, n):
        share(d)
        finish(d - 1)
    finish(n - 1)
    for c in ag:
        c.wait_send()
    for c in so:
        c.wait()


def per_device(
    n, tp,
    hidden, norm_gain, w_query, w_key, w_value, w_gate, w_decay, w_write, decay_rate, head_gain,
    w_output, state, prev_keys, prev_values, prev_decay, prev_write, accepted,
):
    tokens, local = hidden.shape
    width = w_query.shape[1]
    heads = w_decay.shape[1]
    dk = width // heads
    seqs, props = prev_keys.shape[:2]
    owned = tokens // n
    half = owned // 2
    columns = w_output.shape[1]
    R = heads * owned
    chips = tp // 2
    packed = owned // (SMALL // PACK)
    view = state.reshape(seqs, heads, dk, dk).transpose(0, 2, 1, 3).reshape(seqs, dk * heads, dk)
    hbm = pl.BlockSpec(memory_space=pltpu.HBM)
    anyspace = pl.BlockSpec(memory_space=pl.ANY)
    vmem = pl.BlockSpec(memory_space=pltpu.VMEM)
    dma = pltpu.SemaphoreType.DMA
    gain = norm_gain.reshape(-1, 128)
    w_decay, w_write = w_decay.T, w_write.T
    decay_rate, head_gain = decay_rate.reshape(1, -1), head_gain.reshape(1, -1)
    prev_decay, prev_write = prev_decay.transpose(1, 2, 0), prev_write.transpose(1, 2, 0)
    accepted = accepted.reshape(1, -1)
    mixed, state_out = pl.pallas_call(
        functools.partial(kernel, n, tp, norm_gain.shape[0]),
        out_shape=(
            pltpu.VMEM((n, 2, half, columns), BF16),
            pltpu.VMEM(view.shape, F32),
        ),
        in_specs=[hbm] * 17,
        out_specs=(vmem, anyspace),
        scratch_shapes=[
            pltpu.VMEM(hidden.shape, BF16),
            pltpu.VMEM((4,) + w_query.shape, BF16),
            pltpu.VMEM(w_output.shape, BF16),
            pltpu.VMEM((tokens, 4 * width), BF16),
            pltpu.VMEM((n // 2, owned, 4 * width), BF16),
            pltpu.VMEM(view.shape, F32),
            pltpu.VMEM(view.shape, BF16),
            pltpu.VMEM(view.shape, F32),
            pltpu.VMEM((owned, width), F32),
            pltpu.VMEM((2, R, width), BF16),
            pltpu.VMEM((R, dk), F32),
            pltpu.VMEM((R, dk), F32),
            pltpu.VMEM((R, dk), F32),
            pltpu.VMEM((owned, width), BF16),
            pltpu.VMEM((n, owned, width), BF16),
            pltpu.VMEM((n, 2, half, columns), F32),
            pltpu.VMEM((n, 2, half, columns), BF16),
            pltpu.VMEM((n, half, columns), BF16),
            pltpu.VMEM((n, chips, half, columns), BF16),
            pltpu.VMEM((n, 2, half, columns), BF16),
            pltpu.VMEM((n // 2 - 1, owned, 4 * width), BF16),
            pltpu.VMEM((n // 2 - 1, owned, 4 * width), BF16),
            pltpu.VMEM((n, packed, SMALL), F32),
            pltpu.VMEM((n - 1, packed, SMALL), F32),
            pltpu.VMEM(gain.shape, BF16),
            pltpu.VMEM((heads, local), BF16),
            pltpu.VMEM((heads, local), BF16),
            pltpu.VMEM(decay_rate.shape, F32),
            pltpu.VMEM(head_gain.shape, BF16),
            pltpu.VMEM(prev_keys.shape, BF16),
            pltpu.VMEM(prev_values.shape, BF16),
            pltpu.VMEM(prev_decay.shape, F32),
            pltpu.VMEM(prev_write.shape, F32),
            pltpu.VMEM(accepted.shape, jnp.int32),
            dma((6,)), dma((10,)), dma((seqs,)), dma((seqs,)),
            dma((n // 2, 4)), dma((n // 2, 4)), dma((n // 2 - 1, 4)), dma((n // 2 - 1, 4)),
            dma((n - 1,)), dma((n - 1,)), dma((n - 1,)), dma((n,)),
            dma((n,)), dma((n,)), dma((n, chips - 1)), dma((n, chips - 1)), dma((n,)), dma((n,)),
        ],
        compiler_params=pltpu.CompilerParams(
            collective_id=0, has_side_effects=True, vmem_limit_bytes=60 * 2**20
        ),
    )(
        hidden, gain, w_query, w_key, w_value, w_gate, w_decay, w_write,
        decay_rate, head_gain, w_output, view, prev_keys, prev_values,
        prev_decay, prev_write, accepted,
    )
    state_out = state_out.reshape(seqs, dk, heads, dk).transpose(0, 2, 1, 3)
    return mixed.reshape(tokens, columns), state_out.reshape(state.shape)


def solution(mesh):
    placed = (
        P("grp", "kv"),
        P(),
        P("kv", "tp"),
        P("kv", "tp"),
        P("kv", "tp"),
        P("kv", "tp"),
        P(None, "tp"),
        P(None, "tp"),
        P("tp"),
        P(),
        P("tp", "kv"),
        P(("grp", "kv"), "tp", None),
        P(("grp", "kv"), None, "tp"),
        P(("grp", "kv"), None, "tp"),
        P(("grp", "kv"), None, "tp"),
        P(("grp", "kv"), None, "tp"),
        P(("grp", "kv")),
    )
    return jax.shard_map(
        functools.partial(per_device, mesh.shape["kv"], mesh.shape["tp"]),
        mesh=mesh,
        in_specs=placed,
        out_specs=(P("grp", "kv"), P(("grp", "kv"), "tp", None)),
        check_vma=False,
    )
```
